32 devices in a mesh: gr: 2 (over x), fs: 4 (over z), tp: 4 (over y, core).
Axes of the slice: x: 2, y: 2, z: 4, core: 2. Of those that a mesh axis runs over, the one named last changes fastest.
Arguments:
- prompt_tokens: bfloat16 [4096, 2048], P(('gr', 'fs', 'tp')), may hold values from -60 to 60
- norm_gain: float32 [2048], P(('gr', 'fs')), may hold values from 0.1 to 1.9
- up_master: float32 [2048, 8192], P(('gr', 'fs'), 'tp'), may hold values from -0.125 to 0.125
- down_master: float32 [2048, 8192], P(('gr', 'fs'), 'tp'), may hold values from -0.0625 to 0.0625
Outputs:
- up_served: bfloat16 [2048, 8192], P(None, 'tp')
- down_served: bfloat16 [2048, 8192], P(None, 'tp')
- mlp_output: bfloat16 [4096, 2048], P(('gr', 'fs', 'tp'))
The draws below stay inside these ranges and needn't reach their ends.
All inputs are finite; a program needn't handle non-finite values.
Results may differ from the reference program's by a relative error of at most 0.014.
Values may be sent and summed in bfloat16 or wider, within the bound.
A program may use at most 128 MiB of HBM per device.

```python
import math
import jax
import jax.numpy as jnp
from jax import lax

D = 2048
FF = 8192
TOKENS = 4096
N_TP = 4


def draw_prompt_tokens(key, part):
    entry_key, scale_key = jax.random.split(jax.random.fold_in(key, 17))
    entries = jnp.clip(jax.random.normal(entry_key, (TOKENS, D), jnp.float32), -5.0, 5.0)
    scales = jnp.exp(jax.random.uniform(scale_key, (TOKENS,), jnp.float32, 0.0, jnp.log(10.0)))
    return (entries * scales[:, None]).astype(jnp.bfloat16)


def level_of(key, dims, pieces, least, high):
    def one(axis_at, parts):
        steps = jax.random.uniform(jax.random.fold_in(jax.random.fold_in(key, 6), axis_at), (parts,), jnp.float32, least / len(pieces), high / len(pieces))
        return jnp.repeat(jnp.exp(steps), dims[axis_at] // parts).reshape((-1,) + (1,) * (len(dims) - axis_at - 1))

    level = one(*pieces[0])
    for cut in pieces[1:]:
        level = level * one(*cut)
    return level


def bell_draw(key, dims, spread, reach, shards=(), held_as=jnp.bfloat16):
    result = jax.random.normal(key, dims, jnp.float32) * spread
    if len(shards) > 0:
        result = level_of(key, dims, shards, -0.22, 0.18) * result
    return jnp.clip(result, min=-reach, max=reach).astype(held_as)


def setup_inputs(seed: int = 0) -> dict:
    seeds = jax.random.split(jax.random.key(seed), 5)
    prompt_tokens = draw_prompt_tokens(jax.random.fold_in(seeds[4], 71), 0)
    norm_gain = jnp.clip(1.0 + 0.18 * jax.random.normal(seeds[1], (D,), jnp.float32), 0.1, 1.9)
    up_master = bell_draw(seeds[2], (D, FF), D ** -0.5, 0.125, ((0, 8), (1, 4)), jnp.float32)
    down_master = bell_draw(seeds[3], (D, FF), FF ** -0.5, 0.0625, ((0, 8), (1, 4)), jnp.float32)
    return {"prompt_tokens": prompt_tokens, "norm_gain": norm_gain, "up_master": up_master, "down_master": down_master}


def reference(prompt_tokens, norm_gain, up_master, down_master):
    up_served = (up_master * norm_gain[:, None]).astype(jnp.bfloat16)
    down_served = down_master.astype(jnp.bfloat16)
    floats = prompt_tokens.astype(jnp.float32)
    mean_square = lax.optimization_barrier(lax.optimization_barrier(jnp.mean(floats * floats, axis=1, keepdims=True)))
    normed = (floats * lax.rsqrt(mean_square + 1e-06)).astype(jnp.bfloat16)
    block = math.gcd(TOKENS, 1024)
    width = FF // N_TP
    down_blocks = down_served.reshape(D, N_TP, width).astype(jnp.float32)

    def one_block(rows):
        pre = jnp.dot(rows, up_served, preferred_element_type=jnp.float32)
        hidden = jnp.square(jnp.maximum(pre, 0.0)).astype(jnp.bfloat16)
        split = hidden.reshape(block, N_TP, width).astype(jnp.float32)
        partial_value = jnp.einsum('rkf,dkf->krd', split, down_blocks).astype(jnp.bfloat16)
        partial_value = lax.optimization_barrier(partial_value)
        return lax.optimization_barrier(jnp.sum(partial_value.astype(jnp.float32), axis=0)).astype(jnp.bfloat16)
    outputs = lax.map(one_block, normed.reshape(TOKENS // block, block, D))
    return (up_served, down_served, outputs.reshape(TOKENS, D))
```

```python
import functools

import jax
import jax.numpy as jnp
from jax import lax
from jax.experimental import pallas as pl
from jax.experimental.pallas import tpu as pltpu
from jax.sharding import PartitionSpec as P

MESH = pl.DeviceIdType.MESH
CHUNK_BYTES = 128 * 1024


def pieces_of(rows, most):
    count = max(1, -(-rows // most))
    units = rows // 16
    cuts = [16 * (units * i // count) for i in range(count + 1)]
    return [(a, b - a) for a, b in zip(cuts, cuts[1:])]


def kernel(
    sizes, tok_hbm, gain_ref, up_hbm, down_hbm,
    up_ref, down_ref, out_ref,
    tok_ref, stage, normed, hidden, part, arrived,
    load_sem, tok_send, tok_recv,
    z_recv, right_send, left_send, x_recv, x_send, part_send, part_recv,
):
    n_gr, n_fs, n_tp = sizes
    g, z, t = lax.axis_index("gr"), lax.axis_index("fs"), lax.axis_index("tp")
    rows, width = stage.shape[1:]
    local = tok_ref.shape[0]
    depth = up_ref.shape[0]
    last = n_fs - 1
    has_right, has_left = z < last, z > 0
    masters = (up_ref, down_ref)

    def crossing(numerator):
        return max(16, rows * numerator // 256 * 16)

    most = max(16, CHUNK_BYTES // (2 * width) // 16 * 16)
    x_first = (crossing(3), crossing(2))
    tables = []
    for p in range(2):
        table = pieces_of(rows - x_first[p], most)
        tables.append(table + [(rows - x_first[p], x_first[p])] * 2)

    def at(p, col, zz, k):
        start, size = tables[p][k]
        base = pl.multiple_of((col * n_fs + zz) * rows, rows)
        return masters[p].at[pl.ds(pl.multiple_of(base + start, 16), size), :]

    def count(p):
        return len(tables[p]) - 2

    def z_copy(p, zz, k, right):
        col = 1 - g if k == count(p) + 1 else g
        ref = at(p, col, zz, k)
        send = right_send if right else left_send
        return pltpu.make_async_remote_copy(
            src_ref=ref, dst_ref=ref, send_sem=send.at[p, zz, k], recv_sem=z_recv.at[p, zz, k],
            device_id=(g, jnp.where(has_right, z + 1, z - 1) if right else jnp.where(has_left, z - 1, z + 1), t),
            device_id_type=MESH,
        )

    def x_copy(p, zz, k, col):
        ref = at(p, col, zz, k)
        return pltpu.make_async_remote_copy(
            src_ref=ref, dst_ref=ref, send_sem=x_send.at[p, zz, k], recv_sem=x_recv.at[p, zz, k],
            device_id=(1 - g, z, t), device_id_type=MESH,
        )

    def send_both(p, k):
        pl.when(has_right)(lambda: z_copy(p, z, k, True).start())
        pl.when(has_left)(lambda: z_copy(p, z, k, False).start())

    def own_z(p):
        for k in range(count(p) + 1):
            send_both(p, k)

    def own_x(p):
        x_copy(p, z, count(p), g).start()
        for k in range(count(p)):
            x_copy(p, z, k, g).start()

    def other_xz(p):
        x_copy(p, z, count(p), 1 - g).wait_recv()
        send_both(p, count(p) + 1)

    def slot(p, s):
        from_left, from_right = z - s >= 0, z + s <= last
        for k in range(count(p) + 2):
            def left_in():
                z_copy(p, z - s, k, True).wait_recv()
                if s < last:
                    pl.when(has_right)(lambda: z_copy(p, z - s, k, True).start())
                if k < count(p):
                    x_copy(p, z - s, k, g).start()

            def right_in():
                z_copy(p, z + s, k, False).wait_recv()
                if s < last:
                    pl.when(has_left)(lambda: z_copy(p, z + s, k, False).start())
                if k < count(p):
                    x_copy(p, z + s, k, g).start()

            pl.when(from_left)(left_in)
            pl.when(from_right)(right_in)

    def token_copy(j):
        mine = normed.at[pl.ds(pl.multiple_of(t * local, local), local), :]
        return pltpu.make_async_remote_copy(
            src_ref=mine, dst_ref=mine, send_sem=tok_send.at[j - 1], recv_sem=tok_recv.at[j - 1],
            device_id=(g, z, lax.rem(t + j, n_tp)), device_id_type=MESH,
        )

    def part_copy(block, j):
        to = lax.rem(t + j, n_tp)
        row = pl.ds(pl.multiple_of(block * rows, rows), rows)
        return pltpu.make_async_remote_copy(
            src_ref=part.at[row, pl.ds(pl.multiple_of(to * local, local), local)],
            dst_ref=arrived.at[j - 1, row, :],
            send_sem=part_send.at[block, j - 1], recv_sem=part_recv.at[block, j - 1],
            device_id=(g, z, to), device_id_type=MESH,
        )

    def second(s):
        def one(i, carry):
            other, side = i // 2, lax.rem(i, 2)
            dist = s - other
            zz = z + (2 * side - 1) * dist
            ok = (dist >= 0) & (zz >= 0) & (zz <= last) & ((dist > 0) | (side == 0))

            @pl.when(ok)
            def _():
                @pl.when(other == 1)
                def _():
                    for k in range(count(1)):
                        x_copy(1, zz, k, 1 - g).wait_recv()

                block = jnp.where(other == 1, 1 - g, g) * n_fs + zz
                row = pl.ds(pl.multiple_of(block * rows, rows), rows)
                part[row, :] = lax.dot_general(
                    down_ref[row, :], hidden[...], (((1,), (1,)), ((), ())),
                    preferred_element_type=jnp.float32,
                ).astype(part.dtype)
                for j in range(1, n_tp):
                    part_copy(block, j).start()

            return carry

        lax.fori_loop(0, 4, one, 0)

    loads = [
        pltpu.make_async_copy(up_hbm, stage.at[0], load_sem.at[0]),
        pltpu.make_async_copy(tok_hbm, tok_ref, load_sem.at[1]),
        pltpu.make_async_copy(down_hbm, stage.at[1], load_sem.at[2]),
    ]
    for load in loads:
        load.start()

    barrier = pltpu.get_barrier_semaphore()

    def greet(device):
        pl.semaphore_signal(barrier, inc=1, device_id=device, device_id_type=MESH)

    greet((1 - g, z, t))
    for j in range(1, n_tp):
        greet((g, z, lax.rem(t + j, n_tp)))
    pl.when(has_right)(lambda: greet((g, z + 1, t)))
    pl.when(has_left)(lambda: greet((g, z - 1, t)))

    own = pl.ds(pl.multiple_of((g * n_fs + z) * rows, rows), rows)
    loads[0].wait()
    up_ref[own, :] = (stage[0] * gain_ref[...]).astype(up_ref.dtype)
    pl.semaphore_wait(barrier, n_tp + has_right.astype(jnp.int32) + has_left.astype(jnp.int32))
    own_x(0)
    own_z(0)

    loads[1].wait()
    floats = tok_ref[...].astype(jnp.float32)
    mean_square = jnp.mean(floats * floats, axis=1, keepdims=True)
    normed[pl.ds(pl.multiple_of(t * local, local), local), :] = (
        floats * lax.rsqrt(mean_square + 1e-06)
    ).astype(normed.dtype)
    for j in range(1, n_tp):
        token_copy(j).start()
    other_xz(0)
    loads[2].wait()
    down_ref[own, :] = stage[1].astype(down_ref.dtype)

    for s in range(1, last):
        slot(0, s)
    own_z(1)
    if last > 0:
        slot(0, last)
    own_x(1)

    for zz in range(n_fs):
        for k in range(count(0)):
            x_copy(0, zz, k, 1 - g).wait_recv()
    for j in range(1, n_tp):
        token_copy(j).wait_recv()

    tile = 256

    def first(i, carry):
        columns = pl.ds(pl.multiple_of(i * tile, tile), tile)
        pre = jnp.dot(normed[...], up_ref[:, columns], preferred_element_type=jnp.float32)
        hidden[:, columns] = jnp.square(jnp.maximum(pre, 0.0)).astype(hidden.dtype)
        return carry

    lax.fori_loop(0, width // tile, first, 0)

    other_xz(1)
    second(0)
    for s in range(1, n_fs):
        slot(1, s)
        second(s)
    second(n_fs)

    def arrivals(b, carry):
        for j in range(1, n_tp):
            part_copy(b, j).wait_recv()
        return carry

    lax.fori_loop(0, n_gr * n_fs, arrivals, 0)

    def total(i, carry):
        row = pl.ds(pl.multiple_of(i * 128, 128), 128)
        acc = part[row, pl.ds(pl.multiple_of(t * local, local), local)].astype(jnp.float32)
        for j in range(1, n_tp):
            acc = acc + arrived[j - 1, row, :].astype(jnp.float32)
        out_ref[:, row] = acc.T.astype(out_ref.dtype)
        return carry

    lax.fori_loop(0, depth // 128, total, 0)

    def sent_parts(b, carry):
        for j in range(1, n_tp):
            part_copy(b, j).wait_send()
        return carry

    lax.fori_loop(0, n_gr * n_fs, sent_parts, 0)
    for j in range(1, n_tp):
        token_copy(j).wait_send()

    def sent_blocks(zz, carry):
        for p in range(2):
            for k in range(count(p) + 2):
                pl.when(has_right & (zz <= z))(lambda: z_copy(p, zz, k, True).wait_send())
                pl.when(has_left & (zz >= z))(lambda: z_copy(p, zz, k, False).wait_send())
                if k < count(p):
                    x_copy(p, zz, k, g).wait_send()
                elif k == count(p):
                    pl.when(zz == z)(lambda: x_copy(p, zz, k, g).wait_send())
        return carry

    lax.fori_loop(0, n_fs, sent_blocks, 0)


def solution(mesh):
    n_gr, n_fs, n_tp = (mesh.shape[a] for a in ("gr", "fs", "tp"))

    def on_device(prompt_tokens, norm_gain, up_master, down_master):
        local, depth = prompt_tokens.shape
        rows, width = up_master.shape
        blocks = n_gr * n_fs
        most = 2 + -(-rows // max(16, CHUNK_BYTES // (2 * width) // 16 * 16))
        dma = pltpu.SemaphoreType.DMA
        bf16 = jnp.bfloat16
        anywhere = pl.BlockSpec(memory_space=pl.ANY)
        vmem = pl.BlockSpec(memory_space=pltpu.VMEM)
        return pl.pallas_call(
            functools.partial(kernel, (n_gr, n_fs, n_tp)),
            out_shape=(
                pltpu.VMEM((depth, width), bf16),
                pltpu.VMEM((depth, width), bf16),
                jax.ShapeDtypeStruct((local, depth), bf16),
            ),
            in_specs=[anywhere, vmem, anywhere, anywhere],
            out_specs=(vmem, vmem, vmem),
            scratch_shapes=[
                pltpu.VMEM((local, depth), bf16),
                pltpu.VMEM((2, rows, width), jnp.float32),
                pltpu.VMEM((local * n_tp, depth), bf16),
                pltpu.VMEM((local * n_tp, width), bf16),
                pltpu.VMEM((depth, local * n_tp), bf16),
                pltpu.VMEM((n_tp - 1, depth, local), bf16),
                dma((3,)), dma((n_tp - 1,)), dma((n_tp - 1,)),
                dma((2, n_fs, most)), dma((2, n_fs, most)), dma((2, n_fs, most)),
                dma((2, n_fs, most)), dma((2, n_fs, most)),
                dma((blocks, n_tp - 1)), dma((blocks, n_tp - 1)),
            ],
            compiler_params=pltpu.CompilerParams(
                collective_id=0, has_side_effects=True, vmem_limit_bytes=44 * 2**20
            ),
        )(prompt_tokens, norm_gain[:, None], up_master, down_master)

    placed = (
        P(("gr", "fs", "tp"), None),
        P(("gr", "fs")),
        P(("gr", "fs"), "tp"),
        P(("gr", "fs"), "tp"),
    )
    return jax.shard_map(
        on_device,
        mesh=mesh,
        in_specs=placed,
        out_specs=(P(None, "tp"), P(None, "tp"), P(("gr", "fs", "tp"), None)),
        check_vma=False,
    )
```

```python
import functools

import jax
import jax.numpy as jnp
from jax import lax
from jax.experimental import pallas as pl
from jax.experimental.pallas import tpu as pltpu
from jax.sharding import PartitionSpec as P

MESH = pl.DeviceIdType.MESH
CHUNK_BYTES = 128 * 1024


def pieces_of(rows, most):
    count = max(1, -(-rows // most))
    units = rows // 16
    cuts = [16 * (units * i // count) for i in range(count + 1)]
    return [(a, b - a) for a, b in zip(cuts, cuts[1:])]


def kernel(
    sizes, tok_hbm, gain_ref, up_hbm, down_hbm,
    up_ref, down_ref, out_ref,
    tok_ref, stage, normed, hidden, part, arrived,
    load_sem, tok_send, tok_recv,
    z_recv, right_send, left_send, x_recv, x_send, part_send, part_recv,
):
    n_gr, n_fs, n_tp = sizes
    g, z, t = lax.axis_index("gr"), lax.axis_index("fs"), lax.axis_index("tp")
    rows, width = stage.shape[1:]
    local = tok_ref.shape[0]
    depth = up_ref.shape[0]
    last = n_fs - 1
    has_right, has_left = z < last, z > 0
    masters = (up_ref, down_ref)

    def crossing(numerator):
        return max(16, rows * numerator // 256 * 16)

    most = max(16, CHUNK_BYTES // (2 * width) // 16 * 16)
    x_first = (crossing(3), crossing(2))
    tables = []
    for p in range(2):
        table = pieces_of(rows - x_first[p], most)
        tables.append(table + [(rows - x_first[p], x_first[p])] * 2)

    def at(p, col, zz, k):
        start, size = tables[p][k]
        base = pl.multiple_of((col * n_fs + zz) * rows, rows)
        return masters[p].at[pl.ds(pl.multiple_of(base + start, 16), size), :]

    def count(p):
        return len(tables[p]) - 2

    def z_copy(p, zz, k, right):
        col = 1 - g if k == count(p) + 1 else g
        ref = at(p, col, zz, k)
        send = right_send if right else left_send
        return pltpu.make_async_remote_copy(
            src_ref=ref, dst_ref=ref, send_sem=send.at[p, zz, k], recv_sem=z_recv.at[p, zz, k],
            device_id=(g, jnp.where(has_right, z + 1, z - 1) if right else jnp.where(has_left, z - 1, z + 1), t),
            device_id_type=MESH,
        )

    def x_copy(p, zz, k, col):
        ref = at(p, col, zz, k)
        return pltpu.make_async_remote_copy(
            src_ref=ref, dst_ref=ref, send_sem=x_send.at[p, zz, k], recv_sem=x_recv.at[p, zz, k],
            device_id=(1 - g, z, t), device_id_type=MESH,
        )

    def send_both(p, k):
        pl.when(has_right)(lambda: z_copy(p, z, k, True).start())
        pl.when(has_left)(lambda: z_copy(p, z, k, False).start())

    def own_z(p):
        for k in range(count(p) + 1):
            send_both(p, k)

    def own_x(p):
        x_copy(p, z, count(p), g).start()
        for k in range(count(p)):
            x_copy(p, z, k, g).start()

    def other_xz(p):
        x_copy(p, z, count(p), 1 - g).wait_recv()
        send_both(p, count(p) + 1)

    def slot(p, s, items=None):
        from_left, from_right = z - s >= 0, z + s <= last
        for k in range(count(p) + 2) if items is None else items:
            def left_in():
                z_copy(p, z - s, k, True).wait_recv()
                if s < last:
                    pl.when(has_right)(lambda: z_copy(p, z - s, k, True).start())
                if k < count(p):
                    x_copy(p, z - s, k, g).start()

            def right_in():
                z_copy(p, z + s, k, False).wait_recv()
                if s < last:
                    pl.when(has_left)(lambda: z_copy(p, z + s, k, False).start())
                if k < count(p):
                    x_copy(p, z + s, k, g).start()

            pl.when(from_left)(left_in)
            pl.when(from_right)(right_in)

    def token_copy(j):
        mine = normed.at[pl.ds(pl.multiple_of(t * local, local), local), :]
        return pltpu.make_async_remote_copy(
            src_ref=mine, dst_ref=mine, send_sem=tok_send.at[j - 1], recv_sem=tok_recv.at[j - 1],
            device_id=(g, z, lax.rem(t + j, n_tp)), device_id_type=MESH,
        )

    far = jnp.where(z + z >= last, 0, last)
    splits = (0, count(1) * 4 // 7, count(1) * 6 // 7, count(1))
    starts = [tables[1][k][0] for k in splits[:3]] + [rows]
    shares = [(a, b - a) for a, b in zip(starts, starts[1:])]
    whole_block = (0, rows)

    def part_copy(block, share, i, j):
        to = lax.rem(t + j, n_tp)
        start, size = share
        base = pl.multiple_of(block * rows, rows)
        row = pl.ds(pl.multiple_of(base + start, 16), size)
        return pltpu.make_async_remote_copy(
            src_ref=part.at[row, pl.ds(pl.multiple_of(to * local, local), local)],
            dst_ref=arrived.at[j - 1, row, :],
            send_sem=part_send.at[block, i, j - 1], recv_sem=part_recv.at[block, i, j - 1],
            device_id=(g, z, to), device_id_type=MESH,
        )

    def multiply(block, share, i):
        start, size = share
        base = pl.multiple_of(block * rows, rows)
        row = pl.ds(pl.multiple_of(base + start, 16), size)
        part[row, :] = lax.dot_general(
            down_ref[row, :], hidden[...], (((1,), (1,)), ((), ())),
            preferred_element_type=jnp.float32,
        ).astype(part.dtype)
        for j in range(1, n_tp):
            part_copy(block, share, i, j).start()

    def second(s):
        def one(i, carry):
            other, side = i // 2, lax.rem(i, 2)
            dist = s - other
            zz = z + (2 * side - 1) * dist
            ok = (dist >= 0) & (zz >= 0) & (zz <= last) & ((dist > 0) | (side == 0)) & (zz != far)

            @pl.when(ok)
            def _():
                @pl.when(other == 1)
                def _():
                    for k in range(count(1)):
                        x_copy(1, zz, k, 1 - g).wait_recv()

                multiply(jnp.where(other == 1, 1 - g, g) * n_fs + zz, whole_block, 0)

            return carry

        lax.fori_loop(0, 4, one, 0)

    def far_share(col, i):
        if shares[i][1] > 0:
            multiply(col * n_fs + far, shares[i], i)

    def far_x(i):
        for k in range(splits[i], splits[i + 1]):
            x_copy(1, far, k, 1 - g).wait_recv()

    def far_blocks():
        slot(1, last, range(splits[0], splits[1]))
        second(last)
        far_share(g, 0)
        slot(1, last, range(splits[1], splits[2]))
        far_x(0)
        far_share(1 - g, 0)
        far_share(g, 1)
        slot(1, last, range(splits[2], splits[3] + 1))
        far_share(g, 2)
        far_x(1)
        far_share(1 - g, 1)
        slot(1, last, range(splits[3] + 1, splits[3] + 2))
        far_x(2)
        far_share(1 - g, 2)

    def parts(b, act):
        @pl.when(lax.rem(b, n_fs) == far)
        def _():
            for i in range(3):
                if shares[i][1] > 0:
                    for j in range(1, n_tp):
                        act(part_copy(b, shares[i], i, j))

        @pl.when(lax.rem(b, n_fs) != far)
        def _():
            for j in range(1, n_tp):
                act(part_copy(b, whole_block, 0, j))

    loads = [
        pltpu.make_async_copy(up_hbm, stage.at[0], load_sem.at[0]),
        pltpu.make_async_copy(tok_hbm, tok_ref, load_sem.at[1]),
        pltpu.make_async_copy(down_hbm, stage.at[1], load_sem.at[2]),
    ]
    for load in loads:
        load.start()

    barrier = pltpu.get_barrier_semaphore()

    def greet(device):
        pl.semaphore_signal(barrier, inc=1, device_id=device, device_id_type=MESH)

    greet((1 - g, z, t))
    for j in range(1, n_tp):
        greet((g, z, lax.rem(t + j, n_tp)))
    pl.when(has_right)(lambda: greet((g, z + 1, t)))
    pl.when(has_left)(lambda: greet((g, z - 1, t)))

    own = pl.ds(pl.multiple_of((g * n_fs + z) * rows, rows), rows)
    square = (rows, rows)
    on_diagonal = lax.broadcasted_iota(jnp.int32, square, 0) == lax.broadcasted_iota(jnp.int32, square, 1)
    gain = jnp.sum(jnp.where(on_diagonal, gain_ref[...], 0.0), axis=1, keepdims=True)
    loads[0].wait()
    up_ref[own, :] = (stage[0] * gain).astype(up_ref.dtype)
    pl.semaphore_wait(barrier, n_tp + has_right.astype(jnp.int32) + has_left.astype(jnp.int32))
    own_x(0)
    own_z(0)

    loads[1].wait()
    floats = tok_ref[...].astype(jnp.float32)
    mean_square = jnp.mean(floats * floats, axis=1, keepdims=True)
    normed[pl.ds(pl.multiple_of(t * local, local), local), :] = (
        floats * lax.rsqrt(mean_square + 1e-06)
    ).astype(normed.dtype)
    for j in range(1, n_tp):
        token_copy(j).start()
    other_xz(0)
    loads[2].wait()
    down_ref[own, :] = stage[1].astype(down_ref.dtype)

    for s in range(1, last):
        slot(0, s)
    own_z(1)
    if last > 0:
        slot(0, last)
    own_x(1)

    for zz in range(n_fs):
        for k in range(count(0)):
            x_copy(0, zz, k, 1 - g).wait_recv()
    for j in range(1, n_tp):
        token_copy(j).wait_recv()

    tile = 256

    def first(i, carry):
        columns = pl.ds(pl.multiple_of(i * tile, tile), tile)
        pre = jnp.dot(normed[...], up_ref[:, columns], preferred_element_type=jnp.float32)
        hidden[:, columns] = jnp.square(jnp.maximum(pre, 0.0)).astype(hidden.dtype)
        return carry

    lax.fori_loop(0, width // tile, first, 0)

    other_xz(1)
    second(0)
    for s in range(1, last):
        slot(1, s)
        second(s)
    far_blocks()

    final = (1 - g) * n_fs + far
    last_tile = (final * rows + rows - 1) // 128

    def arrivals(b, carry):
        @pl.when(b != final)
        def _():
            parts(b, lambda copy: copy.wait_recv())

        return carry

    lax.fori_loop(0, n_gr * n_fs, arrivals, 0)
    for i in range(2):
        if shares[i][1] > 0:
            for j in range(1, n_tp):
                part_copy(final, shares[i], i, j).wait_recv()

    def total(i, carry):
        row = pl.ds(pl.multiple_of(i * 128, 128), 128)
        acc = part[row, pl.ds(pl.multiple_of(t * local, local), local)].astype(jnp.float32)
        for j in range(1, n_tp):
            acc = acc + arrived[j - 1, row, :].astype(jnp.float32)
        out_ref[:, row] = acc.T.astype(out_ref.dtype)
        return carry

    lax.fori_loop(0, last_tile, total, 0)
    lax.fori_loop(last_tile + 1, depth // 128, total, 0)

    def sent_parts(b, carry):
        parts(b, lambda copy: copy.wait_send())
        return carry

    lax.fori_loop(0, n_gr * n_fs, sent_parts, 0)
    for j in range(1, n_tp):
        token_copy(j).wait_send()

    def sent_blocks(zz, carry):
        for p in range(2):
            for k in range(count(p) + 2):
                pl.when(has_right & (zz <= z))(lambda: z_copy(p, zz, k, True).wait_send())
                pl.when(has_left & (zz >= z))(lambda: z_copy(p, zz, k, False).wait_send())
                if k < count(p):
                    x_copy(p, zz, k, g).wait_send()
                elif k == count(p):
                    pl.when(zz == z)(lambda: x_copy(p, zz, k, g).wait_send())
        return carry

    lax.fori_loop(0, n_fs, sent_blocks, 0)

    for j in range(1, n_tp):
        part_copy(final, shares[2], 2, j).wait_recv()
    total(last_tile, 0)


def solution(mesh):
    n_gr, n_fs, n_tp = (mesh.shape[a] for a in ("gr", "fs", "tp"))

    def on_device(prompt_tokens, norm_gain, up_master, down_master):
        local, depth = prompt_tokens.shape
        rows, width = up_master.shape
        blocks = n_gr * n_fs
        most = 2 + -(-rows // max(16, CHUNK_BYTES // (2 * width) // 16 * 16))
        dma = pltpu.SemaphoreType.DMA
        bf16 = jnp.bfloat16
        anywhere = pl.BlockSpec(memory_space=pl.ANY)
        vmem = pl.BlockSpec(memory_space=pltpu.VMEM)
        return pl.pallas_call(
            functools.partial(kernel, (n_gr, n_fs, n_tp)),
            out_shape=(
                pltpu.VMEM((depth, width), bf16),
                pltpu.VMEM((depth, width), bf16),
                jax.ShapeDtypeStruct((local, depth), bf16),
            ),
            in_specs=[anywhere, vmem, anywhere, anywhere],
            out_specs=(vmem, vmem, vmem),
            scratch_shapes=[
                pltpu.VMEM((local, depth), bf16),
                pltpu.VMEM((2, rows, width), jnp.float32),
                pltpu.VMEM((local * n_tp, depth), bf16),
                pltpu.VMEM((local * n_tp, width), bf16),
                pltpu.VMEM((depth, local * n_tp), bf16),
                pltpu.VMEM((n_tp - 1, depth, local), bf16),
                dma((3,)), dma((n_tp - 1,)), dma((n_tp - 1,)),
                dma((2, n_fs, most)), dma((2, n_fs, most)), dma((2, n_fs, most)),
                dma((2, n_fs, most)), dma((2, n_fs, most)),
                dma((blocks, 3, n_tp - 1)), dma((blocks, 3, n_tp - 1)),
            ],
            compiler_params=pltpu.CompilerParams(
                collective_id=0, has_side_effects=True, vmem_limit_bytes=44 * 2**20
            ),
        )(prompt_tokens, norm_gain[None, :], up_master, down_master)

    placed = (
        P(("gr", "fs", "tp"), None),
        P(("gr", "fs")),
        P(("gr", "fs"), "tp"),
        P(("gr", "fs"), "tp"),
    )
    return jax.shard_map(
        on_device,
        mesh=mesh,
        in_specs=placed,
        out_specs=(P(None, "tp"), P(None, "tp"), P(("gr", "fs", "tp"), None)),
        check_vma=False,
    )
```

```python
import functools

import jax
import jax.numpy as jnp
from jax import lax
from jax.experimental import pallas as pl
from jax.experimental.pallas import tpu as pltpu
from jax.sharding import PartitionSpec as P

MESH = pl.DeviceIdType.MESH
CHUNK_BYTES = 256 * 1024


def pieces_of(rows, most):
    count = max(1, -(-rows // most))
    units = rows // 16
    cuts = [16 * (units * i // count) for i in range(count + 1)]
    return [(a, b - a) for a, b in zip(cuts, cuts[1:])]


def kernel(
    sizes, tok_hbm, gain_ref, up_hbm, down_hbm,
    up_ref, down_ref, out_ref,
    tok_ref, stage, normed, hidden, part, arrived,
    load_sem, tok_send, tok_recv,
    z_recv, right_send, left_send, x_recv, x_send, part_send, part_recv,
):
    n_gr, n_fs, n_tp = sizes
    g, z, t = lax.axis_index("gr"), lax.axis_index("fs"), lax.axis_index("tp")
    rows, width = stage.shape[1:]
    local = tok_ref.shape[0]
    depth = up_ref.shape[0]
    last = n_fs - 1
    has_right, has_left = z < last, z > 0
    masters = (up_ref, down_ref)

    def crossing(numerator):
        return max(16, rows * numerator // 256 * 16)

    most = max(16, CHUNK_BYTES // (2 * width) // 16 * 16)
    x_first = (crossing(3), crossing(3))
    tables = []
    for p in range(2):
        table = pieces_of(rows - x_first[p], most)
        tables.append(table + [(rows - x_first[p], x_first[p])] * 2)

    def at(p, col, zz, k):
        start, size = tables[p][k]
        base = pl.multiple_of((col * n_fs + zz) * rows, rows)
        return masters[p].at[pl.ds(pl.multiple_of(base + start, 16), size), :]

    def count(p):
        return len(tables[p]) - 2

    def z_copy(p, zz, k, right):
        col = 1 - g if k == count(p) + 1 else g
        ref = at(p, col, zz, k)
        send = right_send if right else left_send
        return pltpu.make_async_remote_copy(
            src_ref=ref, dst_ref=ref, send_sem=send.at[p, zz, k], recv_sem=z_recv.at[p, zz, k],
            device_id=(g, jnp.where(has_right, z + 1, z - 1) if right else jnp.where(has_left, z - 1, z + 1), t),
            device_id_type=MESH,
        )

    def x_copy(p, zz, k, col):
        ref = at(p, col, zz, k)
        return pltpu.make_async_remote_copy(
            src_ref=ref, dst_ref=ref, send_sem=x_send.at[p, zz, k], recv_sem=x_recv.at[p, zz, k],
            device_id=(1 - g, z, t), device_id_type=MESH,
        )

    def send_both(p, k):
        pl.when(has_right)(lambda: z_copy(p, z, k, True).start())
        pl.when(has_left)(lambda: z_copy(p, z, k, False).start())

    def own_z(p):
        for k in range(count(p) + 1):
            send_both(p, k)

    def own_x(p):
        x_copy(p, z, count(p), g).start()
        for k in range(count(p)):
            x_copy(p, z, k, g).start()

    def other_xz(p):
        x_copy(p, z, count(p), 1 - g).wait_recv()
        send_both(p, count(p) + 1)

    def slot(p, s, items=None):
        from_left, from_right = z - s >= 0, z + s <= last
        for k in range(count(p) + 2) if items is None else items:
            def left_in():
                z_copy(p, z - s, k, True).wait_recv()
                if s < last:
                    pl.when(has_right)(lambda: z_copy(p, z - s, k, True).start())
                if k < count(p):
                    x_copy(p, z - s, k, g).start()

            def right_in():
                z_copy(p, z + s, k, False).wait_recv()
                if s < last:
                    pl.when(has_left)(lambda: z_copy(p, z + s, k, False).start())
                if k < count(p):
                    x_copy(p, z + s, k, g).start()

            pl.when(from_left)(left_in)
            pl.when(from_right)(right_in)

    def token_copy(j):
        mine = normed.at[pl.ds(pl.multiple_of(t * local, local), local), :]
        return pltpu.make_async_remote_copy(
            src_ref=mine, dst_ref=mine, send_sem=tok_send.at[j - 1], recv_sem=tok_recv.at[j - 1],
            device_id=(g, z, lax.rem(t + j, n_tp)), device_id_type=MESH,
        )

    far = jnp.where(z + z >= last, 0, last)
    splits = (0, count(1) * 4 // 7, count(1) * 6 // 7, count(1))
    starts = [tables[1][k][0] for k in splits[:3]] + [rows]
    shares = [(a, b - a) for a, b in zip(starts, starts[1:])]
    whole_block = (0, rows)

    def part_copy(block, share, i, j):
        to = lax.rem(t + j, n_tp)
        start, size = share
        base = pl.multiple_of(block * rows, rows)
        row = pl.ds(pl.multiple_of(base + start, 16), size)
        return pltpu.make_async_remote_copy(
            src_ref=part.at[row, pl.ds(pl.multiple_of(to * local, local), local)],
            dst_ref=arrived.at[j - 1, row, :],
            send_sem=part_send.at[block, i, j - 1], recv_sem=part_recv.at[block, i, j - 1],
            device_id=(g, z, to), device_id_type=MESH,
        )

    def multiply(block, share, i):
        start, size = share
        base = pl.multiple_of(block * rows, rows)
        row = pl.ds(pl.multiple_of(base + start, 16), size)
        part[row, :] = lax.dot_general(
            down_ref[row, :], hidden[...], (((1,), (1,)), ((), ())),
            preferred_element_type=jnp.float32,
        ).astype(part.dtype)
        for j in range(1, n_tp):
            part_copy(block, share, i, j).start()

    def second(s):
        def one(i, carry):
            other, side = i // 2, lax.rem(i, 2)
            dist = s - other
            zz = z + (2 * side - 1) * dist
            ok = (dist >= 0) & (zz >= 0) & (zz <= last) & ((dist > 0) | (side == 0)) & (zz != far)

            @pl.when(ok)
            def _():
                @pl.when(other == 1)
                def _():
                    for k in range(count(1)):
                        x_copy(1, zz, k, 1 - g).wait_recv()

                multiply(jnp.where(other == 1, 1 - g, g) * n_fs + zz, whole_block, 0)

            return carry

        lax.fori_loop(0, 4, one, 0)

    def far_share(col, i):
        if shares[i][1] > 0:
            multiply(col * n_fs + far, shares[i], i)

    def far_x(i):
        for k in range(splits[i], splits[i + 1]):
            x_copy(1, far, k, 1 - g).wait_recv()

    def far_blocks():
        slot(1, last, range(splits[0], splits[1]))
        second(last)
        far_share(g, 0)
        slot(1, last, range(splits[1], splits[2]))
        far_x(0)
        far_share(1 - g, 0)
        far_share(g, 1)
        slot(1, last, range(splits[2], splits[3] + 1))
        far_share(g, 2)
        far_x(1)
        far_share(1 - g, 1)
        slot(1, last, range(splits[3] + 1, splits[3] + 2))
        far_x(2)
        far_share(1 - g, 2)

    def parts(b, act):
        @pl.when(lax.rem(b, n_fs) == far)
        def _():
            for i in range(3):
                if shares[i][1] > 0:
                    for j in range(1, n_tp):
                        act(part_copy(b, shares[i], i, j))

        @pl.when(lax.rem(b, n_fs) != far)
        def _():
            for j in range(1, n_tp):
                act(part_copy(b, whole_block, 0, j))

    loads = [
        pltpu.make_async_copy(up_hbm, stage.at[0], load_sem.at[0]),
        pltpu.make_async_copy(tok_hbm, tok_ref, load_sem.at[1]),
        pltpu.make_async_copy(down_hbm, stage.at[1], load_sem.at[2]),
    ]
    loads[0].start()
    loads[1].start()

    barrier = pltpu.get_barrier_semaphore()

    def greet(device):
        pl.semaphore_signal(barrier, inc=1, device_id=device, device_id_type=MESH)

    greet((1 - g, z, t))
    for j in range(1, n_tp):
        greet((g, z, lax.rem(t + j, n_tp)))
    pl.when(has_right)(lambda: greet((g, z + 1, t)))
    pl.when(has_left)(lambda: greet((g, z - 1, t)))

    def round_up(k):
        start, size = tables[0][k]
        row = pl.ds(pl.multiple_of((g * n_fs + z) * rows + start, 16), size)
        up_ref[row, :] = (stage[0, start : start + size] * gain[start : start + size]).astype(up_ref.dtype)

    def send_own(k):
        x_copy(0, z, k, g).start()
        if k < count(0):
            send_both(0, k)

    own = pl.ds(pl.multiple_of((g * n_fs + z) * rows, rows), rows)
    square = (rows, rows)
    on_diagonal = lax.broadcasted_iota(jnp.int32, square, 0) == lax.broadcasted_iota(jnp.int32, square, 1)
    gain = jnp.sum(jnp.where(on_diagonal, gain_ref[...], 0.0), axis=1, keepdims=True)
    loads[0].wait()
    order = [count(0)] + list(range(count(0)))
    round_up(order[0])
    round_up(order[1])
    pl.semaphore_wait(barrier, n_tp + has_right.astype(jnp.int32) + has_left.astype(jnp.int32))
    for i, k in enumerate(order):
        send_own(k)
        if i + 2 < len(order):
            round_up(order[i + 2])
    send_both(0, count(0))
    loads[2].start()

    loads[1].wait()
    floats = tok_ref[...].astype(jnp.float32)
    mean_square = jnp.mean(floats * floats, axis=1, keepdims=True)
    normed[pl.ds(pl.multiple_of(t * local, local), local), :] = (
        floats * lax.rsqrt(mean_square + 1e-06)
    ).astype(normed.dtype)
    for j in range(1, n_tp):
        token_copy(j).start()
    other_xz(0)
    loads[2].wait()
    down_ref[own, :] = stage[1].astype(down_ref.dtype)

    for s in range(1, last):
        slot(0, s)
    own_z(1)
    if last > 0:
        slot(0, last)
    own_x(1)

    for zz in range(n_fs):
        for k in range(count(0)):
            x_copy(0, zz, k, 1 - g).wait_recv()
    for j in range(1, n_tp):
        token_copy(j).wait_recv()

    tile = 256

    def first(i, carry):
        columns = pl.ds(pl.multiple_of(i * tile, tile), tile)
        pre = jnp.dot(normed[...], up_ref[:, columns], preferred_element_type=jnp.float32)
        hidden[:, columns] = jnp.square(jnp.maximum(pre, 0.0)).astype(hidden.dtype)
        return carry

    lax.fori_loop(0, width // tile, first, 0)

    other_xz(1)
    second(0)
    for s in range(1, last):
        slot(1, s)
        second(s)
    far_blocks()

    final = (1 - g) * n_fs + far
    last_tile = (final * rows + rows - 1) // 128

    def arrivals(b, carry):
        @pl.when(b != final)
        def _():
            parts(b, lambda copy: copy.wait_recv())

        return carry

    lax.fori_loop(0, n_gr * n_fs, arrivals, 0)
    for i in range(2):
        if shares[i][1] > 0:
            for j in range(1, n_tp):
                part_copy(final, shares[i], i, j).wait_recv()

    def total(i, carry):
        row = pl.ds(pl.multiple_of(i * 128, 128), 128)
        acc = part[row, pl.ds(pl.multiple_of(t * local, local), local)].astype(jnp.float32)
        for j in range(1, n_tp):
            acc = acc + arrived[j - 1, row, :].astype(jnp.float32)
        out_ref[:, row] = acc.T.astype(out_ref.dtype)
        return carry

    lax.fori_loop(0, last_tile, total, 0)
    lax.fori_loop(last_tile + 1, depth // 128, total, 0)

    def sent_parts(b, carry):
        parts(b, lambda copy: copy.wait_send())
        return carry

    lax.fori_loop(0, n_gr * n_fs, sent_parts, 0)
    for j in range(1, n_tp):
        token_copy(j).wait_send()

    def sent_blocks(zz, carry):
        for p in range(2):
            for k in range(count(p) + 2):
                pl.when(has_right & (zz <= z))(lambda: z_copy(p, zz, k, True).wait_send())
                pl.when(has_left & (zz >= z))(lambda: z_copy(p, zz, k, False).wait_send())
                if k < count(p):
                    x_copy(p, zz, k, g).wait_send()
                elif k == count(p):
                    pl.when(zz == z)(lambda: x_copy(p, zz, k, g).wait_send())
        return carry

    lax.fori_loop(0, n_fs, sent_blocks, 0)

    for j in range(1, n_tp):
        part_copy(final, shares[2], 2, j).wait_recv()
    total(last_tile, 0)


def solution(mesh):
    n_gr, n_fs, n_tp = (mesh.shape[a] for a in ("gr", "fs", "tp"))

    def on_device(prompt_tokens, norm_gain, up_master, down_master):
        local, depth = prompt_tokens.shape
        rows, width = up_master.shape
        blocks = n_gr * n_fs
        most = 2 + -(-rows // max(16, CHUNK_BYTES // (2 * width) // 16 * 16))
        dma = pltpu.SemaphoreType.DMA
        bf16 = jnp.bfloat16
        anywhere = pl.BlockSpec(memory_space=pl.ANY)
        vmem = pl.BlockSpec(memory_space=pltpu.VMEM)
        return pl.pallas_call(
            functools.partial(kernel, (n_gr, n_fs, n_tp)),
            out_shape=(
                pltpu.VMEM((depth, width), bf16),
                pltpu.VMEM((depth, width), bf16),
                jax.ShapeDtypeStruct((local, depth), bf16),
            ),
            in_specs=[anywhere, vmem, anywhere, anywhere],
            out_specs=(vmem, vmem, vmem),
            scratch_shapes=[
                pltpu.VMEM((local, depth), bf16),
                pltpu.VMEM((2, rows, width), jnp.float32),
                pltpu.VMEM((local * n_tp, depth), bf16),
                pltpu.VMEM((local * n_tp, width), bf16),
                pltpu.VMEM((depth, local * n_tp), bf16),
                pltpu.VMEM((n_tp - 1, depth, local), bf16),
                dma((3,)), dma((n_tp - 1,)), dma((n_tp - 1,)),
                dma((2, n_fs, most)), dma((2, n_fs, most)), dma((2, n_fs, most)),
                dma((2, n_fs, most)), dma((2, n_fs, most)),
                dma((blocks, 3, n_tp - 1)), dma((blocks, 3, n_tp - 1)),
            ],
            compiler_params=pltpu.CompilerParams(
                collective_id=0, has_side_effects=True, vmem_limit_bytes=44 * 2**20
            ),
        )(prompt_tokens, norm_gain[None, :], up_master, down_master)

    placed = (
        P(("gr", "fs", "tp"), None),
        P(("gr", "fs")),
        P(("gr", "fs"), "tp"),
        P(("gr", "fs"), "tp"),
    )
    return jax.shard_map(
        on_device,
        mesh=mesh,
        in_specs=placed,
        out_specs=(P(None, "tp"), P(None, "tp"), P(("gr", "fs", "tp"), None)),
        check_vma=False,
    )
```
